32 devices in a mesh: sp: 8 (over z, core), tp: 4 (over y, x).
Axes of the slice: x: 2, y: 2, z: 4, core: 2. Of those that a mesh axis runs over, the one named last changes fastest.
Arguments:
- queries: bfloat16 [2048, 2048], P('sp', 'tp'), may hold values from -8 to 8
- key_rows: bfloat16 [2048, 1024], P('sp', 'tp'), may hold values from -8 to 8
- values: bfloat16 [2048, 1024], P('sp', 'tp'), may hold values from -6 to 6
- sink_logits: float32 [32], P('tp'), may hold values from 2 to 6
- residual: bfloat16 [2048, 2048], P(('sp', 'tp')), may hold values from -6 to 6
- out_weight: bfloat16 [2048, 2048], P('tp'), may hold values from -0.125 to 0.125
- norm_gain: float32 [2048], replicated, may hold values from 0.1 to 1.9
- expert_ids: int32 [2048, 2], P('sp'), may hold values from 0 to 7, as said below
- route_weight: float32 [2048, 2], P('sp'), may hold values from 0.2 to 1
- gate_proj: bfloat16 [8, 2048, 4096], P('sp', None, 'tp'), may hold values from -0.125 to 0.125
- up_proj: bfloat16 [8, 2048, 4096], P('sp', None, 'tp'), may hold values from -0.125 to 0.125
- down_proj: bfloat16 [8, 4096, 2048], P('sp', 'tp'), may hold values from -0.09375 to 0.09375
Outputs:
- mixed_out: bfloat16 [2048, 2048], P(('sp', 'tp'))
The draws below stay inside these ranges and needn't reach their ends.
Inputs may be any that keep to these rules, and one draw needn't show every extreme that they name: `expert_ids`: the two entries of a row are different experts of one group: experts g * 2 to g * 2 + 1 for a group g below 4. In each aligned block of 64 rows (the rows of one device) no expert is named more than 32 times, and one expert is named exactly 32 times in every block.
All inputs are finite; a program needn't handle non-finite values.
Results may differ from the reference program's by a relative error of at most 0.014.
Values may be sent and summed in bfloat16 or wider, within the bound.
A program may use at most 64 MiB of HBM per device.

```python
import math
import jax
import jax.numpy as jnp
from jax import lax

D = 2048
HEAD = 64
QH = 32
KVH = 16
WINDOW = 128
FFE = 4096
TOK_SP = 256
CAP = 32
SEQ = 2048
EXPERTS = 8
INNER = 2
N_SP = 8
N_TP = 4


def draw_queries(key, part):
    sampled = jnp.clip(jax.random.normal(jax.random.fold_in(key, 3), (SEQ, QH * HEAD), jnp.float32), -5.5, 5.5)
    return sampled.astype(jnp.bfloat16)


def draw_key_rows(key, part):
    sampled = jnp.clip(jax.random.normal(jax.random.fold_in(key, 8), (SEQ, KVH * HEAD), jnp.float32), -5.5, 5.5)
    return sampled.astype(jnp.bfloat16)


def draw_expert_ids(key, part):
    rows_per = TOK_SP // N_TP
    block_count = SEQ // rows_per
    favour = jax.random.randint(jax.random.fold_in(key, 5), (N_SP,), 0, 1500)
    jitter = jax.random.randint(jax.random.fold_in(key, 6), (block_count, rows_per, 2, N_SP), 0, 1000)
    forced = jax.random.randint(jax.random.fold_in(key, 7), (), 0, N_SP)
    labels = jnp.arange(N_SP, dtype=jnp.int32)
    family = labels // INNER
    same_family = (family[:, None] == family[None, :]).astype(jnp.int32)

    def one_block(block_jitter):

        def place(counts, entry_item):
            position, random_draws = entry_item
            has_room = (counts < CAP).astype(jnp.int32)
            family_room = jnp.sum(same_family * has_room[None, :], 1)
            usable = (has_room > 0) & (family_room >= 2)
            ranking = (random_draws[0] + favour) * N_SP + labels
            ranking = jnp.where((labels == forced) & (position < CAP), 100000000, ranking)
            ranking = jnp.where(usable, ranking, -1)
            first_pick = jnp.argmax(ranking).astype(jnp.int32)
            usable_two = (has_room > 0) & (family == family[first_pick]) & (labels != first_pick)
            ranking_two = jnp.where(usable_two, (random_draws[1] + favour) * N_SP + labels, -1)
            second = jnp.argmax(ranking_two).astype(jnp.int32)
            counts = counts + (labels == first_pick).astype(jnp.int32) + (labels == second).astype(jnp.int32)
            return (counts, jnp.stack([first_pick, second]))
        ignored, chosen = lax.scan(place, jnp.zeros((N_SP,), jnp.int32), (jnp.arange(rows_per, dtype=jnp.int32), block_jitter))
        return chosen
    return jax.vmap(one_block)(jitter).reshape(SEQ, 2).astype(jnp.int32)


def block_levels(key, dims, split, smallest, top_value):
    loudness, own = 1.0, jax.random.fold_in(key, 6)
    for axis_at, parts in split:
        draws = jnp.exp(jax.random.uniform(jax.random.fold_in(own, axis_at), (parts,), jnp.float32, smallest / len(split), top_value / len(split)))
        loudness = loudness * jnp.repeat(draws, dims[axis_at] // parts).reshape([-1 if axis == axis_at else 1 for axis in range(len(dims))])
    return loudness


def bell_draw(key, dims, spread, reach, pieces=(), kind=jnp.bfloat16):
    values = spread * jax.random.normal(key, dims, jnp.float32)
    if pieces:
        values = values * block_levels(key, dims, pieces, -0.22, 0.18)
    return jnp.clip(values, -reach, reach).astype(kind)


def setup_inputs(seed: int = 0) -> dict:
    splits = jax.random.split(jax.random.key(seed), 13)
    return {
        "queries": draw_queries(jax.random.fold_in(splits[12], 71), 0),
        "key_rows": draw_key_rows(jax.random.fold_in(splits[12], 71), 0),
        "values": bell_draw(splits[2], (SEQ, KVH * HEAD), 1.0, 6.0, ((0, 8), (1, 4))),
        "sink_logits": jnp.clip(2.0 + 4.0 * jax.random.uniform(splits[3], (QH,), jnp.float32) ** block_levels(splits[3], (QH,), ((0, 4),), -0.2, 0.2), 2.0, 6.0),
        "residual": bell_draw(splits[4], (SEQ, D), 1.0, 6.0, ((0, 32),)),
        "out_weight": bell_draw(splits[5], (QH * HEAD, D), (QH * HEAD) ** -0.5, 0.125, ((0, 4),)),
        "norm_gain": jnp.clip(1.0 + 0.18 * jax.random.normal(splits[6], (D,), jnp.float32), 0.1, 1.9),
        "expert_ids": draw_expert_ids(jax.random.fold_in(splits[12], 71), 0),
        "route_weight": jnp.clip(jnp.exp(math.log(1.0) - 1.609438 * jax.random.uniform(splits[8], (SEQ, 2), jnp.float32) ** block_levels(splits[8], (SEQ, 2), ((0, 8),), -0.2, 0.2)), 0.2, 1.0),
        "gate_proj": bell_draw(splits[9], (EXPERTS, D, FFE), D ** -0.5, 0.125, ((0, 8), (2, 4))),
        "up_proj": bell_draw(splits[10], (EXPERTS, D, FFE), D ** -0.5, 0.125, ((0, 8), (2, 4))),
        "down_proj": bell_draw(splits[11], (EXPERTS, FFE, D), FFE ** -0.5, 0.09375, ((0, 8), (1, 4))),
    }


norm_epsilon = 1e-06

def rotary(values_in, positions, head_count):
    halfway = HEAD // 2
    frequency = 10000.0 ** (-jnp.arange(halfway, dtype=jnp.float32) * 2.0 / HEAD)
    angles = positions.astype(jnp.float32)[:, None] * frequency[None, :]
    cosine = jnp.cos(angles)[:, None, :]
    sine_part = jnp.sin(angles)[:, None, :]
    reshaped = values_in.astype(jnp.float32).reshape(values_in.shape[0], head_count, HEAD)
    front_part = reshaped[..., :halfway]
    back_part = reshaped[..., halfway:]
    turned = jnp.concatenate([front_part * cosine - back_part * sine_part, back_part * cosine + front_part * sine_part], -1)
    return turned.astype(jnp.bfloat16)

def attend(query_blocks, key_pairs, value_pairs, sink_grid, key_start):
    block_count = query_blocks.shape[0]
    window_len = query_blocks.shape[1]
    scores = jnp.einsum('bqkgd,bskd->bkgqs', query_blocks.astype(jnp.float32), key_pairs.astype(jnp.float32)) * HEAD ** (-0.5)
    row_idx = jnp.arange(window_len)[:, None]
    col_idx = jnp.arange(2 * window_len)[None, :]
    distance = row_idx - col_idx + window_len
    key_pos = key_start + jnp.arange(block_count)[:, None, None] * window_len + col_idx[None]
    allowed = (distance >= 0)[None] & (distance < window_len)[None] & (key_pos >= 0)
    scores = jnp.where(allowed[:, None, None], scores, -jnp.inf)
    sink_full = sink_grid.astype(jnp.float32)[None, :, :, None]
    highest = jnp.maximum(lax.optimization_barrier(jnp.max(scores, -1)), sink_full)
    exp_scores = jnp.exp(scores - highest[..., None])
    denominator = lax.optimization_barrier(jnp.sum(exp_scores, -1)) + jnp.exp(sink_full - highest)
    probs = lax.optimization_barrier(exp_scores.astype(jnp.bfloat16)).astype(jnp.float32)
    weighted = jnp.einsum('bkgqs,bskd->bkgqd', probs, value_pairs.astype(jnp.float32))
    normalized = weighted / denominator[..., None]
    return jnp.transpose(normalized, (0, 3, 1, 2, 4)).astype(jnp.bfloat16).reshape(block_count * window_len, -1)

def reference(queries, key_rows, values, sink_logits, residual, out_weight, norm_gain, expert_ids, route_weight, gate_proj, up_proj, down_proj):
    seq_len = queries.shape[0]
    positions = jnp.arange(seq_len, dtype=jnp.int32)
    rot_query = rotary(queries, positions, QH)
    rot_key = rotary(key_rows, positions, KVH)
    group_size = QH // KVH
    block_count = seq_len // WINDOW
    padding = jnp.zeros((WINDOW, KVH, HEAD), jnp.bfloat16)
    key_blocks = jnp.concatenate([padding, rot_key], 0).reshape(block_count + 1, WINDOW, KVH, HEAD)
    value_blocks = jnp.concatenate([padding, values.reshape(seq_len, KVH, HEAD)], 0).reshape(block_count + 1, WINDOW, KVH, HEAD)
    key_pairs = jnp.concatenate([key_blocks[:-1], key_blocks[1:]], 1)
    value_pairs = jnp.concatenate([value_blocks[:-1], value_blocks[1:]], 1)
    query_blocks = rot_query.reshape(block_count, WINDOW, KVH, group_size, HEAD)
    sink_grid = sink_logits.reshape(KVH, group_size)

    def one_head(entry_item):
        query_part, key_part, value_part, sink_part = entry_item
        return attend(query_part[:, :, None], key_part[:, :, None], value_part[:, :, None], sink_part[None], -WINDOW)
    per_head = lax.map(one_head, (jnp.moveaxis(query_blocks, 2, 0), jnp.moveaxis(key_pairs, 2, 0), jnp.moveaxis(value_pairs, 2, 0), sink_grid))
    attended = jnp.moveaxis(per_head, 0, 1).reshape(seq_len, QH * HEAD)
    middle = (residual.astype(jnp.float32) + jnp.dot(attended, out_weight, preferred_element_type=jnp.float32)).astype(jnp.bfloat16)
    middle_f = middle.astype(jnp.float32)
    normed = (middle_f * lax.rsqrt(lax.optimization_barrier(jnp.mean(middle_f * middle_f, -1, keepdims=True)) + norm_epsilon) * norm_gain).astype(jnp.bfloat16)
    flattened = expert_ids.reshape(-1).astype(jnp.int32)
    most_rows = N_SP * N_TP * CAP
    slice_width = FFE // N_TP

    def one_expert(expert_index):
        matches = flattened == expert_index
        located = jnp.nonzero(matches, size=most_rows, fill_value=0)[0].astype(jnp.int32)
        is_live = jnp.arange(most_rows) < jnp.sum(matches.astype(jnp.int32))
        rows_in = normed[located // 2]
        gate_val = jnp.dot(rows_in, gate_proj[expert_index], preferred_element_type=jnp.float32)
        up_val = jnp.dot(rows_in, up_proj[expert_index], preferred_element_type=jnp.float32)
        hidden = lax.optimization_barrier((jax.nn.silu(gate_val) * up_val).astype(jnp.bfloat16)).astype(jnp.float32)
        down_slices = down_proj[expert_index].astype(jnp.float32).reshape(N_TP, slice_width, -1)
        slice_out = jnp.einsum('rsf,sfd->srd', hidden.reshape(most_rows, N_TP, slice_width), down_slices)
        slice_out = lax.optimization_barrier(slice_out.astype(jnp.bfloat16)).astype(jnp.float32)
        summed = lax.optimization_barrier(jnp.sum(slice_out, 0))
        return (located, summed * is_live[:, None].astype(jnp.float32))
    all_located, all_outputs = lax.map(one_expert, jnp.arange(N_SP, dtype=jnp.int32))
    assigned = jnp.zeros((seq_len * 2, normed.shape[1]), jnp.float32).at[all_located.reshape(-1)].add(all_outputs.reshape(-1, normed.shape[1]))
    routed = lax.optimization_barrier(jnp.sum(assigned.reshape(seq_len, 2, -1) * route_weight[..., None], 1))
    return (middle_f + routed).astype(jnp.bfloat16)
```

```python
import jax
import jax.numpy as jnp
from jax import lax
from jax.experimental import pallas as pl
from jax.experimental.pallas import tpu as pltpu
from jax.sharding import PartitionSpec as P

HEAD = 64
WINDOW = 128


norm_epsilon = 1e-06


def from_behind(block, axis, distance):
    devices = range(lax.axis_size(axis))
    route = [(i - distance, i) for i in devices if i - distance in devices]
    return lax.ppermute(block, axis, route)


def rotary(values_in, positions, head_count):
    halfway = HEAD // 2
    frequency = 10000.0 ** (-jnp.arange(halfway, dtype=jnp.float32) * 2.0 / HEAD)
    angles = positions.astype(jnp.float32)[:, None] * frequency[None, :]
    cosine = jnp.cos(angles)[:, None, :]
    sine_part = jnp.sin(angles)[:, None, :]
    reshaped = values_in.astype(jnp.float32).reshape(values_in.shape[0], head_count, HEAD)
    front_part = reshaped[..., :halfway]
    back_part = reshaped[..., halfway:]
    turned = jnp.concatenate(
        [front_part * cosine - back_part * sine_part, back_part * cosine + front_part * sine_part],
        -1,
    )
    return turned.astype(jnp.bfloat16)


def attend(query_blocks, key_pairs, value_pairs, sink_grid, key_start):
    block_count = query_blocks.shape[0]
    window_len = query_blocks.shape[1]
    scores = jnp.einsum(
        "bqkgd,bskd->bkgqs", query_blocks, key_pairs, preferred_element_type=jnp.float32
    ) * HEAD ** (-0.5)
    row_idx = jnp.arange(window_len)[:, None]
    col_idx = jnp.arange(2 * window_len)[None, :]
    distance = row_idx - col_idx + window_len
    key_pos = key_start + jnp.arange(block_count)[:, None, None] * window_len + col_idx[None]
    allowed = (distance >= 0)[None] & (distance < window_len)[None] & (key_pos >= 0)
    scores = jnp.where(allowed[:, None, None], scores, -jnp.inf)
    sink_full = sink_grid[None, :, :, None]
    highest = jnp.maximum(jnp.max(scores, -1), sink_full)
    exp_scores = jnp.exp(scores - highest[..., None])
    denominator = jnp.sum(exp_scores, -1) + jnp.exp(sink_full - highest)
    weighted = jnp.einsum(
        "bkgqs,bskd->bkgqd",
        exp_scores.astype(jnp.bfloat16),
        value_pairs,
        preferred_element_type=jnp.float32,
    )
    normalized = weighted / denominator[..., None]
    return (
        jnp.transpose(normalized, (0, 3, 1, 2, 4))
        .astype(jnp.bfloat16)
        .reshape(block_count * window_len, -1)
    )


def slot_select(picks_in, expert_count, capacity):
    flattened = picks_in.reshape(-1)
    onehot = (flattened[:, None] == jnp.arange(expert_count, dtype=jnp.int32)[None, :]).astype(
        jnp.int32
    )
    rank_of = jnp.sum(jnp.cumsum(onehot, 0) * onehot, 1) - 1
    slot_of = flattened * capacity + rank_of
    chosen = jnp.arange(expert_count * capacity, dtype=jnp.int32)[:, None] == slot_of[None, :]
    return chosen.astype(jnp.bfloat16)


def expert_part(rows_in, gate_proj, up_proj, down_proj):
    in_shape = rows_in.shape
    flattened = rows_in.reshape(-1, in_shape[-1])
    gate_val = jnp.dot(flattened, gate_proj[0], preferred_element_type=jnp.float32)
    up_val = jnp.dot(flattened, up_proj[0], preferred_element_type=jnp.float32)
    hidden = (jax.nn.silu(gate_val) * up_val).astype(jnp.bfloat16)
    return (
        jnp.dot(hidden, down_proj[0], preferred_element_type=jnp.float32)
        .astype(jnp.bfloat16)
        .reshape(in_shape)
    )


GROUPS = 4
TILE = 256
MESH = pl.DeviceIdType.MESH


def group_kernel(
    proj, resid, gain, extra, sel, sel_back, wg_hbm, wu_hbm, wd_hbm, out,
    wg, wu, wd, w_sem,
    rs_in, rs_s, rs_r,
    mid, normed, outb, rows,
    di_s, di_r, ag_s, ag_r, pt_s, pt_r,
    hid, outp, pr, pr_s, pr_r,
    comb, rs2, r2_s, r2_r,
    ret, back, bk_s, bk_r,
):
    sp = lax.axis_index("sp")
    t = lax.axis_index("tp")
    core = lax.rem(sp, 2)
    z = sp // 2
    tp_n, row_n, width = proj.shape
    ext_width = normed.shape[1]
    cap = outb.shape[1]
    half = GROUPS * cap
    flip1 = t + 1 - 2 * lax.rem(t, 2)
    flip2 = lax.rem(t + 2, 4)
    flip3 = lax.rem(flip1 + 2, 4)
    peer = [t, flip1, flip2, flip3]
    partner = sp + 1 - 2 * core
    zoff = lambda k: lax.rem(z + k + GROUPS, GROUPS)

    loads = [
        pltpu.make_async_copy(a, b, w_sem.at[i])
        for i, (a, b) in enumerate(((wg_hbm, wg), (wu_hbm, wu), (wd_hbm, wd)))
    ]
    for c in loads:
        c.start()

    barrier = pltpu.get_barrier_semaphore()
    friends = [(sp, peer[d]) for d in (1, 2, 3)]
    friends += [(zoff(k) * 2 + core, t) for k in (1, 2, 3)] + [(partner, t)]
    for dev in friends:
        pl.semaphore_signal(barrier, inc=1, device_id=dev, device_id_type=MESH)
    pl.semaphore_wait(barrier, len(friends))

    sent = []

    def send(src, dst, ss, rs, dev):
        c = pltpu.make_async_remote_copy(
            src_ref=src, dst_ref=dst, send_sem=ss, recv_sem=rs, device_id=dev, device_id_type=MESH
        )
        c.start()
        sent.append(c)
        return c

    firsts = [
        send(proj.at[peer[d]], rs_in.at[d - 1], rs_s.at[d - 1], rs_r.at[d - 1], (sp, peer[d]))
        for d in (3, 1, 2)
    ]
    for c in firsts:
        c.wait_recv()
    total = resid[...].astype(jnp.float32) + (
        proj[t].astype(jnp.float32)
        + rs_in[0].astype(jnp.float32)
        + rs_in[1].astype(jnp.float32)
        + rs_in[2].astype(jnp.float32)
    )
    middle = total.astype(jnp.bfloat16)
    mid[...] = middle
    mf = middle.astype(jnp.float32)
    scale = lax.rsqrt(jnp.mean(mf * mf, -1, keepdims=True) + norm_epsilon)
    normed[:, :width] = (mf * scale * gain[...]).astype(jnp.bfloat16)
    normed[:, width:] = extra[...]

    def block(tt, cc, zz):
        return rows.at[tt, pl.ds(pl.multiple_of((cc * GROUPS + zz) * cap, cap), cap)]

    def pack(g):
        s = sel[pl.ds(pl.multiple_of(g * cap, cap), cap), :]
        return jnp.dot(s, normed[...], preferred_element_type=jnp.float32).astype(jnp.bfloat16)

    disp = [None] * GROUPS
    for k in (2, 1, 3):
        g = zoff(k)
        outb[k] = pack(g)
        disp[k] = send(
            outb.at[k], block(t, core, z), di_s.at[k - 1], di_r.at[k - 1], (2 * g + core, t)
        )
    block(t, core, z)[...] = pack(z)

    ag = {}
    pt = {}

    def push(d, k, tt, to):
        ref = block(tt, core, zoff(-k))
        ag[(d, k)] = send(ref, ref, ag_s.at[d - 1, k], ag_r.at[d - 1, k], (sp, peer[to]))

    def across(d, k):
        ref = block(peer[d], core, zoff(-k))
        pt[(d, k)] = send(ref, ref, pt_s.at[d, k], pt_r.at[d, k], (partner, t))

    order = (0, 1, 3, 2)

    def relay(i):
        k = order[i]
        ag[(1, k)].wait_recv()
        if i < 2:
            push(3, k, peer[1], 2)
        across(1, k)
        ag[(2, k)].wait_recv()
        if i >= 2:
            push(3, k, peer[2], 1)
        across(2, k)

    for i, k in enumerate(order):
        if k:
            disp[k].wait_recv()
        push(1, k, t, 1)
        push(2, k, t, 2)
        across(0, k)
        if i:
            relay(i - 1)

    for c in loads:
        c.wait()

    def experts(d):
        for k in order:
            pt[(d, k)].wait_recv()
        tt = peer[d]

        @pl.loop(0, wg.shape[1] // TILE)
        def _(n):
            cols = pl.ds(pl.multiple_of(n * TILE, TILE), TILE)
            x = rows[tt, :, :width]
            g = jnp.dot(x, wg[:, cols], preferred_element_type=jnp.float32)
            u = jnp.dot(x, wu[:, cols], preferred_element_type=jnp.float32)
            hid[:, cols] = (g / (1.0 + jnp.exp(-g)) * u).astype(jnp.bfloat16)

        ext = rows[tt, :, width:].astype(jnp.float32)
        lane = lax.broadcasted_iota(jnp.int32, ext.shape, 1)
        mine = (lane == core) | (lane == core + 2)
        weight = jnp.sum(jnp.where(mine, ext, 0.0), -1, keepdims=True)

        @pl.loop(0, width // TILE)
        def _(n):
            cols = pl.ds(pl.multiple_of(n * TILE, TILE), TILE)
            y = jnp.dot(hid[...], wd[:, cols], preferred_element_type=jnp.float32)
            outp[d, :, cols] = (y * weight).astype(jnp.bfloat16)

        src = outp.at[d, pl.ds(pl.multiple_of((1 - core) * half, half), half)]
        return send(src, pr.at[d], pr_s.at[d], pr_r.at[d], (partner, t))

    def own(d, zz):
        off = pl.multiple_of((core * GROUPS + zz) * cap, cap)
        here = pl.ds(pl.multiple_of(zz * cap, cap), cap)
        return outp[d, pl.ds(off, cap), :].astype(jnp.float32) + pr[d, here, :].astype(jnp.float32)

    back_order = (2, 1, 3, 0)
    r2 = {}

    def combine(d, swap):
        swap.wait_recv()
        for k in back_order:
            zz = zoff(-k)
            comb[d - 1, k] = own(d, zz).astype(jnp.bfloat16)
            r2[(d, k)] = send(
                comb.at[d - 1, k], rs2.at[d - 1, k],
                r2_s.at[d - 1, k], r2_r.at[d - 1, k], (sp, peer[d]),
            )

    swap0 = experts(0)
    relay(3)
    swap1 = experts(1)
    swap0.wait_recv()
    for k in order:
        ag[(3, k)].wait_recv()
        across(3, k)
    combine(1, swap1)
    swap2 = experts(2)
    combine(2, swap2)
    swap3 = experts(3)
    combine(3, swap3)

    bk = []
    for k in back_order:
        zz = zoff(-k)
        acc = own(0, zz)
        for d in (1, 2, 3):
            r2[(d, k)].wait_recv()
            acc = acc + rs2[d - 1, k].astype(jnp.float32)
        if k:
            ret[k] = acc.astype(jnp.bfloat16)
            bk.append(
                send(ret.at[k], back.at[z], bk_s.at[k - 1], bk_r.at[k - 1], (2 * zz + core, t))
            )
        else:
            back[z] = acc.astype(jnp.bfloat16)
    for c in bk:
        c.wait_recv()
    routed = jnp.dot(
        sel_back[...], back[...].reshape(half, width), preferred_element_type=jnp.float32
    )
    out[...] = (mid[...].astype(jnp.float32) + routed).astype(jnp.bfloat16)
    for c in sent:
        c.wait_send()


def group_experts(projected, residual, norm_gain, own_ids, own_weights, gate, up, down):
    row_n, width = residual.shape
    tp_n = lax.axis_size("tp")
    expert_n = lax.axis_size("sp")
    cap = 2 * max(1, 2 * row_n // expert_n)
    group = own_ids[:, 0] // 2
    onehot = (group[:, None] == jnp.arange(GROUPS, dtype=jnp.int32)[None, :]).astype(jnp.int32)
    rank_of = jnp.sum(jnp.cumsum(onehot, 0) * onehot, 1) - 1
    slot = group * cap + rank_of
    hit = jnp.arange(GROUPS * cap, dtype=jnp.int32)[:, None] == slot[None, :]
    sel = hit.astype(jnp.bfloat16)
    odd = lax.rem(own_ids, 2)
    pair = jnp.stack(
        [jnp.sum(jnp.where(odd == p, own_weights, 0.0), 1) for p in (0, 1)], 1
    )
    high = pair.astype(jnp.bfloat16)
    low = (pair - high.astype(jnp.float32)).astype(jnp.bfloat16)
    extra = jnp.pad(jnp.concatenate([high, low], 1), ((0, 0), (0, 124)))
    ext_width = width + 128
    ff = gate.shape[-1]
    half = GROUPS * cap
    bf = jnp.bfloat16
    dma = pltpu.SemaphoreType.DMA
    vmem = pl.BlockSpec(memory_space=pltpu.VMEM)
    hbm = pl.BlockSpec(memory_space=pl.ANY)
    return pl.pallas_call(
        group_kernel,
        out_shape=jax.ShapeDtypeStruct((row_n, width), bf),
        in_specs=[vmem] * 6 + [hbm] * 3,
        out_specs=vmem,
        scratch_shapes=[
            pltpu.VMEM((width, ff), bf),
            pltpu.VMEM((width, ff), bf),
            pltpu.VMEM((ff, width), bf),
            dma((3,)),
            pltpu.VMEM((3, row_n, width), bf),
            dma((3,)),
            dma((3,)),
            pltpu.VMEM((row_n, width), bf),
            pltpu.VMEM((row_n, ext_width), bf),
            pltpu.VMEM((GROUPS, cap, ext_width), bf),
            pltpu.VMEM((tp_n, 2 * half, ext_width), bf),
            dma((3,)),
            dma((3,)),
            dma((3, GROUPS)),
            dma((3, GROUPS)),
            dma((4, GROUPS)),
            dma((4, GROUPS)),
            pltpu.VMEM((2 * half, ff), bf),
            pltpu.VMEM((4, 2 * half, width), bf),
            pltpu.VMEM((4, half, width), bf),
            dma((4,)),
            dma((4,)),
            pltpu.VMEM((3, GROUPS, cap, width), bf),
            pltpu.VMEM((3, GROUPS, cap, width), bf),
            dma((3, GROUPS)),
            dma((3, GROUPS)),
            pltpu.VMEM((GROUPS, cap, width), bf),
            pltpu.VMEM((GROUPS, cap, width), bf),
            dma((3,)),
            dma((3,)),
        ],
        compiler_params=pltpu.CompilerParams(
            collective_id=0, has_side_effects=True, vmem_limit_bytes=56 * 2**20
        ),
    )(
        projected.reshape(tp_n, row_n, width), residual, norm_gain[None], extra, sel,
        sel.T, gate[0], up[0], down[0],
    )


def per_device(
    queries,
    key_rows,
    values,
    sink_logits,
    residual,
    out_weight,
    norm_gain,
    expert_ids,
    route_weight,
    gate_proj,
    up_proj,
    down_proj,
):
    local_len = queries.shape[0]
    q_heads = sink_logits.shape[0]
    kv_heads = key_rows.shape[1] // HEAD
    group_size = q_heads // kv_heads
    window_len = WINDOW
    seq_start = lax.axis_index("sp") * local_len
    rim_pair = jnp.stack([key_rows[local_len - window_len :], values[local_len - window_len :]])
    rim_pair = from_behind(rim_pair, "sp", 1)
    key_ext = jnp.concatenate([rim_pair[0], key_rows], 0)
    val_ext = jnp.concatenate([rim_pair[1], values], 0)
    positions = seq_start + jnp.arange(local_len, dtype=jnp.int32)
    ext_positions = seq_start - window_len + jnp.arange(local_len + window_len, dtype=jnp.int32)
    rot_query = rotary(queries, positions, q_heads)
    rot_key = rotary(key_ext, ext_positions, kv_heads)
    block_count = local_len // window_len
    query_blocks = rot_query.reshape(block_count, window_len, kv_heads, group_size, HEAD)
    key_blocks = rot_key.reshape(block_count + 1, window_len, kv_heads, HEAD)
    value_blocks = val_ext.reshape(block_count + 1, window_len, kv_heads, HEAD)
    key_pairs = jnp.concatenate([key_blocks[:-1], key_blocks[1:]], 1)
    value_pairs = jnp.concatenate([value_blocks[:-1], value_blocks[1:]], 1)
    sink_grid = sink_logits.reshape(kv_heads, group_size)
    attended = attend(query_blocks, key_pairs, value_pairs, sink_grid, seq_start - window_len)
    tok_rows = residual.shape[0]
    tp_count = lax.axis_size("tp")
    tp_index = lax.axis_index("tp")
    if tp_count == 4 and lax.axis_size("sp") == 2 * GROUPS:
        return group_experts(
            jnp.dot(attended, out_weight, preferred_element_type=jnp.float32).astype(
                jnp.bfloat16
            ),
            residual,
            norm_gain,
            lax.dynamic_slice_in_dim(expert_ids, tp_index * tok_rows, tok_rows, 0),
            lax.dynamic_slice_in_dim(route_weight, tp_index * tok_rows, tok_rows, 0),
            gate_proj,
            up_proj,
            down_proj,
        )
    projected = lax.psum_scatter(
        jnp.dot(attended, out_weight, preferred_element_type=jnp.float32).astype(jnp.bfloat16),
        "tp",
        scatter_dimension=0,
        tiled=True,
    ).astype(jnp.float32)
    middle = (residual.astype(jnp.float32) + projected).astype(jnp.bfloat16)
    middle_f = middle.astype(jnp.float32)
    normed = (
        middle_f
        * lax.rsqrt(jnp.mean(middle_f * middle_f, -1, keepdims=True) + norm_epsilon)
        * norm_gain
    ).astype(jnp.bfloat16)
    expert_count = lax.axis_size("sp")
    capacity = 2 * max(1, 2 * tok_rows // expert_count)
    model_width = normed.shape[1]
    own_ids = lax.dynamic_slice_in_dim(expert_ids, tp_index * tok_rows, tok_rows, 0)
    own_weights = lax.dynamic_slice_in_dim(route_weight, tp_index * tok_rows, tok_rows, 0)
    select = slot_select(own_ids, expert_count, capacity)
    token_select = jnp.sum(select.reshape(expert_count * capacity, tok_rows, 2), -1)
    outbound = jnp.dot(token_select, normed, preferred_element_type=jnp.float32).astype(
        jnp.bfloat16
    )
    outbound = outbound.reshape(expert_count, capacity, model_width)
    arrived = lax.all_to_all(outbound, "sp", split_axis=0, concat_axis=0, tiled=True)
    partial_out = expert_part(
        lax.all_gather(arrived, "tp", axis=0, tiled=True), gate_proj, up_proj, down_proj
    )
    partial_out = partial_out.reshape(tp_count, expert_count * capacity, model_width)
    width_parts = lax.all_to_all(partial_out, "tp", split_axis=0, concat_axis=0, tiled=True)
    summed = jnp.sum(width_parts.astype(jnp.float32), 0).reshape(
        expert_count, capacity, model_width
    )
    returned = (
        lax.all_to_all(summed.astype(jnp.bfloat16), "sp", split_axis=0, concat_axis=0, tiled=True)
        .astype(summed.dtype)
        .reshape(expert_count * capacity, model_width)
    )
    picked = jnp.dot(
        select.astype(jnp.float32).T,
        returned,
        precision=lax.Precision.HIGHEST,
        preferred_element_type=jnp.float32,
    )
    routed = jnp.sum(picked.reshape(tok_rows, 2, model_width) * own_weights[..., None], 1)
    return (middle_f + routed).astype(jnp.bfloat16)


def solution(mesh):
    return jax.shard_map(
        per_device,
        mesh=mesh,
        in_specs=(
            P("sp", "tp"),
            P("sp", "tp"),
            P("sp", "tp"),
            P("tp"),
            P(("sp", "tp"), None),
            P("tp", None),
            P(),
            P("sp", None),
            P("sp", None),
            P("sp", None, "tp"),
            P("sp", None, "tp"),
            P("sp", "tp", None),
        ),
        out_specs=P(("sp", "tp"), None),
        check_vma=False,
    )
```

```python
import jax
import jax.numpy as jnp
from jax import lax
from jax.experimental import pallas as pl
from jax.experimental.pallas import tpu as pltpu
from jax.sharding import PartitionSpec as P

HEAD = 64
WINDOW = 128


norm_epsilon = 1e-06


def from_behind(block, axis, distance):
    devices = range(lax.axis_size(axis))
    route = [(i - distance, i) for i in devices if i - distance in devices]
    return lax.ppermute(block, axis, route)


def rotary(values_in, positions, head_count):
    halfway = HEAD // 2
    frequency = 10000.0 ** (-jnp.arange(halfway, dtype=jnp.float32) * 2.0 / HEAD)
    angles = positions.astype(jnp.float32)[:, None] * frequency[None, :]
    cosine = jnp.cos(angles)[:, None, :]
    sine_part = jnp.sin(angles)[:, None, :]
    reshaped = values_in.astype(jnp.float32).reshape(values_in.shape[0], head_count, HEAD)
    front_part = reshaped[..., :halfway]
    back_part = reshaped[..., halfway:]
    turned = jnp.concatenate(
        [front_part * cosine - back_part * sine_part, back_part * cosine + front_part * sine_part],
        -1,
    )
    return turned.astype(jnp.bfloat16)


def attend(query_blocks, key_pairs, value_pairs, sink_grid, key_start):
    block_count = query_blocks.shape[0]
    window_len = query_blocks.shape[1]
    scores = jnp.einsum(
        "bqkgd,bskd->bkgqs", query_blocks, key_pairs, preferred_element_type=jnp.float32
    ) * HEAD ** (-0.5)
    row_idx = jnp.arange(window_len)[:, None]
    col_idx = jnp.arange(2 * window_len)[None, :]
    distance = row_idx - col_idx + window_len
    key_pos = key_start + jnp.arange(block_count)[:, None, None] * window_len + col_idx[None]
    allowed = (distance >= 0)[None] & (distance < window_len)[None] & (key_pos >= 0)
    scores = jnp.where(allowed[:, None, None], scores, -jnp.inf)
    sink_full = sink_grid[None, :, :, None]
    highest = jnp.maximum(jnp.max(scores, -1), sink_full)
    exp_scores = jnp.exp(scores - highest[..., None])
    denominator = jnp.sum(exp_scores, -1) + jnp.exp(sink_full - highest)
    weighted = jnp.einsum(
        "bkgqs,bskd->bkgqd",
        exp_scores.astype(jnp.bfloat16),
        value_pairs,
        preferred_element_type=jnp.float32,
    )
    normalized = weighted / denominator[..., None]
    return (
        jnp.transpose(normalized, (0, 3, 1, 2, 4))
        .astype(jnp.bfloat16)
        .reshape(block_count * window_len, -1)
    )


def slot_select(picks_in, expert_count, capacity):
    flattened = picks_in.reshape(-1)
    onehot = (flattened[:, None] == jnp.arange(expert_count, dtype=jnp.int32)[None, :]).astype(
        jnp.int32
    )
    rank_of = jnp.sum(jnp.cumsum(onehot, 0) * onehot, 1) - 1
    slot_of = flattened * capacity + rank_of
    chosen = jnp.arange(expert_count * capacity, dtype=jnp.int32)[:, None] == slot_of[None, :]
    return chosen.astype(jnp.bfloat16)


def expert_part(rows_in, gate_proj, up_proj, down_proj):
    in_shape = rows_in.shape
    flattened = rows_in.reshape(-1, in_shape[-1])
    gate_val = jnp.dot(flattened, gate_proj[0], preferred_element_type=jnp.float32)
    up_val = jnp.dot(flattened, up_proj[0], preferred_element_type=jnp.float32)
    hidden = (jax.nn.silu(gate_val) * up_val).astype(jnp.bfloat16)
    return (
        jnp.dot(hidden, down_proj[0], preferred_element_type=jnp.float32)
        .astype(jnp.bfloat16)
        .reshape(in_shape)
    )


GROUPS = 4
TILE = 256
MESH = pl.DeviceIdType.MESH


def group_kernel(
    proj, resid, gain, extra, sel, sel_back, wg_hbm, wu_hbm, wd_hbm, out,
    wg, wu, wd, w_sem,
    rs_in, rs_s, rs_r,
    mid, normed, outb, rows,
    di_s, di_r, ag_s, ag_r, pt_s, pt_r,
    hid, outp, pr, pr_s, pr_r,
    comb, rs2, r2_s, r2_r,
    ret, back, bk_s, bk_r,
):
    sp = lax.axis_index("sp")
    t = lax.axis_index("tp")
    core = lax.rem(sp, 2)
    z = sp // 2
    tp_n, row_n, width = proj.shape
    ext_width = normed.shape[1]
    cap = outb.shape[1]
    half = GROUPS * cap
    flip1 = t + 1 - 2 * lax.rem(t, 2)
    flip2 = lax.rem(t + 2, 4)
    flip3 = lax.rem(flip1 + 2, 4)
    peer = [t, flip1, flip2, flip3]
    partner = sp + 1 - 2 * core
    zoff = lambda k: lax.rem(z + k + GROUPS, GROUPS)

    loads = [
        pltpu.make_async_copy(a, b, w_sem.at[i])
        for i, (a, b) in enumerate(((wg_hbm, wg), (wu_hbm, wu), (wd_hbm, wd)))
    ]
    for c in loads:
        c.start()

    barrier = pltpu.get_barrier_semaphore()
    friends = [(sp, peer[d]) for d in (1, 2, 3)]
    friends += [(zoff(k) * 2 + core, t) for k in (1, 2, 3)] + [(partner, t)]
    for dev in friends:
        pl.semaphore_signal(barrier, inc=1, device_id=dev, device_id_type=MESH)
    pl.semaphore_wait(barrier, len(friends))

    sent = []

    def send(src, dst, ss, rs, dev):
        c = pltpu.make_async_remote_copy(
            src_ref=src, dst_ref=dst, send_sem=ss, recv_sem=rs, device_id=dev, device_id_type=MESH
        )
        c.start()
        sent.append(c)
        return c

    firsts = [
        send(proj.at[peer[d]], rs_in.at[d - 1], rs_s.at[d - 1], rs_r.at[d - 1], (sp, peer[d]))
        for d in (3, 1, 2)
    ]
    for c in firsts:
        c.wait_recv()
    total = resid[...].astype(jnp.float32) + (
        proj[t].astype(jnp.float32)
        + rs_in[0].astype(jnp.float32)
        + rs_in[1].astype(jnp.float32)
        + rs_in[2].astype(jnp.float32)
    )
    middle = total.astype(jnp.bfloat16)
    mid[...] = middle
    mf = middle.astype(jnp.float32)
    scale = lax.rsqrt(jnp.mean(mf * mf, -1, keepdims=True) + norm_epsilon)
    normed[:, :width] = (mf * scale * gain[...]).astype(jnp.bfloat16)
    normed[:, width:] = extra[...]

    def block(tt, cc, zz):
        return rows.at[zz, pl.ds(pl.multiple_of((cc * tp_n + tt) * cap, cap), cap)]

    def pack(g):
        s = sel[pl.ds(pl.multiple_of(g * cap, cap), cap), :]
        return jnp.dot(s, normed[...], preferred_element_type=jnp.float32).astype(jnp.bfloat16)

    order = (0, 1, 3, 2)
    ag = {}
    pt = {}

    def push(d, k, tt, to):
        ref = block(tt, core, zoff(-k))
        ag[(d, k)] = send(ref, ref, ag_s.at[d - 1, k], ag_r.at[d - 1, k], (sp, peer[to]))

    def across(d, k):
        ref = block(peer[d], core, zoff(-k))
        pt[(d, k)] = send(ref, ref, pt_s.at[d, k], pt_r.at[d, k], (partner, t))

    disp = [None] * GROUPS

    def spread(i):
        k = order[i]
        if k:
            disp[k].wait_recv()
        push(1, k, t, 1)
        push(2, k, t, 2)
        across(0, k)

    def relay(i):
        k = order[i]
        via = 1 + i % 2
        ag[(via, k)].wait_recv()
        push(3, k, peer[via], 3 - via)
        across(via, k)
        ag[(3 - via, k)].wait_recv()
        across(3 - via, k)

    def corner(i):
        k = order[i]
        ag[(3, k)].wait_recv()
        across(3, k)

    def widen(i):
        k = order[i]
        zz = zoff(-k)
        for d in (0, 1, 2, 3):
            pt[(d, k)].wait_recv()

        @pl.loop(0, wg.shape[1] // TILE)
        def _(n):
            cols = pl.ds(pl.multiple_of(n * TILE, TILE), TILE)
            x = rows[zz, :, :width]
            g = jnp.dot(x, wg[:, cols], preferred_element_type=jnp.float32)
            u = jnp.dot(x, wu[:, cols], preferred_element_type=jnp.float32)
            hid[:, cols] = (g / (1.0 + jnp.exp(-g)) * u).astype(jnp.bfloat16)

    swap = {}

    def narrow(i):
        k = order[i]
        ext = rows[zoff(-k), :, width:].astype(jnp.float32)
        lane = lax.broadcasted_iota(jnp.int32, ext.shape, 1)
        mine = (lane == core) | (lane == core + 2)
        weight = jnp.sum(jnp.where(mine, ext, 0.0), -1, keepdims=True)

        @pl.loop(0, width // TILE)
        def _(n):
            cols = pl.ds(pl.multiple_of(n * TILE, TILE), TILE)
            y = jnp.dot(hid[...], wd[:, cols], preferred_element_type=jnp.float32)
            outp[k, :, cols] = (y * weight).astype(jnp.bfloat16)

        other = outp.at[k, pl.ds(pl.multiple_of((1 - core) * half, half), half)]
        swap[k] = send(other, pr.at[k], pr_s.at[k], pr_r.at[k], (partner, t))

    def own(k, d):
        off = pl.multiple_of((core * tp_n + peer[d]) * cap, cap)
        here = pl.ds(pl.multiple_of(peer[d] * cap, cap), cap)
        return outp[k, pl.ds(off, cap), :].astype(jnp.float32) + pr[k, here, :].astype(jnp.float32)

    r2 = {}

    def ship(k, d, to):
        r2[(d, k)] = send(
            comb.at[k, d - 1], rs2.at[k, d - 1],
            r2_s.at[d - 1, k], r2_r.at[d - 1, k], (sp, peer[to]),
        )

    def combine(i):
        k = order[i]
        via = 1 + i % 2
        swap[k].wait_recv()
        comb[k, 2] = own(k, 3).astype(jnp.bfloat16)
        ship(k, 3, via)
        comb[k, via - 1] = own(k, via).astype(jnp.bfloat16)
        ship(k, via, via)

    def combine_on(i):
        k = order[i]
        on = 2 - i % 2
        r2[(3, k)].wait_recv()
        comb[k, on - 1] = (own(k, on) + rs2[k, 2].astype(jnp.float32)).astype(jnp.bfloat16)
        ship(k, on, on)

    bk = []

    def finish(i):
        k = order[i]
        acc = own(k, 0)
        for d in (1, 2):
            r2[(d, k)].wait_recv()
            acc = acc + rs2[k, d - 1].astype(jnp.float32)
        if k:
            ret[k] = acc.astype(jnp.bfloat16)
            bk.append(
                send(
                    ret.at[k], back.at[z], bk_s.at[k - 1], bk_r.at[k - 1],
                    (2 * zoff(-k) + core, t),
                )
            )
        else:
            back[z] = acc.astype(jnp.bfloat16)

    block(t, core, z)[...] = pack(z)
    spread(0)
    for k in (1, 3, 2):
        g = zoff(k)
        outb[k] = pack(g)
        disp[k] = send(
            outb.at[k], block(t, core, z), di_s.at[k - 1], di_r.at[k - 1], (2 * g + core, t)
        )
    relay(0)
    corner(0)
    spread(1)
    for c in loads:
        c.wait()
    widen(0)
    relay(1)
    spread(2)
    narrow(0)
    corner(1)
    widen(1)
    relay(2)
    spread(3)
    combine(0)
    narrow(1)
    corner(2)
    widen(2)
    relay(3)
    combine_on(0)
    combine(1)
    narrow(2)
    corner(3)
    combine_on(1)
    widen(3)
    finish(0)
    combine(2)
    narrow(3)
    finish(1)
    combine_on(2)
    combine(3)
    finish(2)
    combine_on(3)
    finish(3)
    for c in bk:
        c.wait_recv()
    routed = jnp.dot(
        sel_back[...], back[...].reshape(half, width), preferred_element_type=jnp.float32
    )
    out[...] = (mid[...].astype(jnp.float32) + routed).astype(jnp.bfloat16)
    for c in sent:
        c.wait_send()


def group_experts(projected, residual, norm_gain, own_ids, own_weights, gate, up, down):
    row_n, width = residual.shape
    tp_n = lax.axis_size("tp")
    expert_n = lax.axis_size("sp")
    cap = 2 * max(1, 2 * row_n // expert_n)
    group = own_ids[:, 0] // 2
    onehot = (group[:, None] == jnp.arange(GROUPS, dtype=jnp.int32)[None, :]).astype(jnp.int32)
    rank_of = jnp.sum(jnp.cumsum(onehot, 0) * onehot, 1) - 1
    slot = group * cap + rank_of
    hit = jnp.arange(GROUPS * cap, dtype=jnp.int32)[:, None] == slot[None, :]
    sel = hit.astype(jnp.bfloat16)
    odd = lax.rem(own_ids, 2)
    pair = jnp.stack(
        [jnp.sum(jnp.where(odd == p, own_weights, 0.0), 1) for p in (0, 1)], 1
    )
    high = pair.astype(jnp.bfloat16)
    low = (pair - high.astype(jnp.float32)).astype(jnp.bfloat16)
    extra = jnp.pad(jnp.concatenate([high, low], 1), ((0, 0), (0, 124)))
    ext_width = width + 128
    ff = gate.shape[-1]
    half = GROUPS * cap
    bf = jnp.bfloat16
    dma = pltpu.SemaphoreType.DMA
    vmem = pl.BlockSpec(memory_space=pltpu.VMEM)
    hbm = pl.BlockSpec(memory_space=pl.ANY)
    return pl.pallas_call(
        group_kernel,
        out_shape=jax.ShapeDtypeStruct((row_n, width), bf),
        in_specs=[vmem] * 6 + [hbm] * 3,
        out_specs=vmem,
        scratch_shapes=[
            pltpu.VMEM((width, ff), bf),
            pltpu.VMEM((width, ff), bf),
            pltpu.VMEM((ff, width), bf),
            dma((3,)),
            pltpu.VMEM((3, row_n, width), bf),
            dma((3,)),
            dma((3,)),
            pltpu.VMEM((row_n, width), bf),
            pltpu.VMEM((row_n, ext_width), bf),
            pltpu.VMEM((GROUPS, cap, ext_width), bf),
            pltpu.VMEM((GROUPS, 2 * half, ext_width), bf),
            dma((3,)),
            dma((3,)),
            dma((3, GROUPS)),
            dma((3, GROUPS)),
            dma((4, GROUPS)),
            dma((4, GROUPS)),
            pltpu.VMEM((2 * half, ff), bf),
            pltpu.VMEM((4, 2 * half, width), bf),
            pltpu.VMEM((4, half, width), bf),
            dma((4,)),
            dma((4,)),
            pltpu.VMEM((GROUPS, 3, cap, width), bf),
            pltpu.VMEM((GROUPS, 3, cap, width), bf),
            dma((3, GROUPS)),
            dma((3, GROUPS)),
            pltpu.VMEM((GROUPS, cap, width), bf),
            pltpu.VMEM((GROUPS, cap, width), bf),
            dma((3,)),
            dma((3,)),
        ],
        compiler_params=pltpu.CompilerParams(
            collective_id=0, has_side_effects=True, vmem_limit_bytes=56 * 2**20
        ),
    )(
        projected.reshape(tp_n, row_n, width), residual, norm_gain[None], extra, sel,
        sel.T, gate[0], up[0], down[0],
    )


def per_device(
    queries,
    key_rows,
    values,
    sink_logits,
    residual,
    out_weight,
    norm_gain,
    expert_ids,
    route_weight,
    gate_proj,
    up_proj,
    down_proj,
):
    local_len = queries.shape[0]
    q_heads = sink_logits.shape[0]
    kv_heads = key_rows.shape[1] // HEAD
    group_size = q_heads // kv_heads
    window_len = WINDOW
    seq_start = lax.axis_index("sp") * local_len
    rim_pair = jnp.stack([key_rows[local_len - window_len :], values[local_len - window_len :]])
    rim_pair = from_behind(rim_pair, "sp", 1)
    key_ext = jnp.concatenate([rim_pair[0], key_rows], 0)
    val_ext = jnp.concatenate([rim_pair[1], values], 0)
    positions = seq_start + jnp.arange(local_len, dtype=jnp.int32)
    ext_positions = seq_start - window_len + jnp.arange(local_len + window_len, dtype=jnp.int32)
    rot_query = rotary(queries, positions, q_heads)
    rot_key = rotary(key_ext, ext_positions, kv_heads)
    block_count = local_len // window_len
    query_blocks = rot_query.reshape(block_count, window_len, kv_heads, group_size, HEAD)
    key_blocks = rot_key.reshape(block_count + 1, window_len, kv_heads, HEAD)
    value_blocks = val_ext.reshape(block_count + 1, window_len, kv_heads, HEAD)
    key_pairs = jnp.concatenate([key_blocks[:-1], key_blocks[1:]], 1)
    value_pairs = jnp.concatenate([value_blocks[:-1], value_blocks[1:]], 1)
    sink_grid = sink_logits.reshape(kv_heads, group_size)
    attended = attend(query_blocks, key_pairs, value_pairs, sink_grid, seq_start - window_len)
    tok_rows = residual.shape[0]
    tp_count = lax.axis_size("tp")
    tp_index = lax.axis_index("tp")
    if tp_count == 4 and lax.axis_size("sp") == 2 * GROUPS:
        return group_experts(
            jnp.dot(attended, out_weight, preferred_element_type=jnp.float32).astype(
                jnp.bfloat16
            ),
            residual,
            norm_gain,
            lax.dynamic_slice_in_dim(expert_ids, tp_index * tok_rows, tok_rows, 0),
            lax.dynamic_slice_in_dim(route_weight, tp_index * tok_rows, tok_rows, 0),
            gate_proj,
            up_proj,
            down_proj,
        )
    projected = lax.psum_scatter(
        jnp.dot(attended, out_weight, preferred_element_type=jnp.float32).astype(jnp.bfloat16),
        "tp",
        scatter_dimension=0,
        tiled=True,
    ).astype(jnp.float32)
    middle = (residual.astype(jnp.float32) + projected).astype(jnp.bfloat16)
    middle_f = middle.astype(jnp.float32)
    normed = (
        middle_f
        * lax.rsqrt(jnp.mean(middle_f * middle_f, -1, keepdims=True) + norm_epsilon)
        * norm_gain
    ).astype(jnp.bfloat16)
    expert_count = lax.axis_size("sp")
    capacity = 2 * max(1, 2 * tok_rows // expert_count)
    model_width = normed.shape[1]
    own_ids = lax.dynamic_slice_in_dim(expert_ids, tp_index * tok_rows, tok_rows, 0)
    own_weights = lax.dynamic_slice_in_dim(route_weight, tp_index * tok_rows, tok_rows, 0)
    select = slot_select(own_ids, expert_count, capacity)
    token_select = jnp.sum(select.reshape(expert_count * capacity, tok_rows, 2), -1)
    outbound = jnp.dot(token_select, normed, preferred_element_type=jnp.float32).astype(
        jnp.bfloat16
    )
    outbound = outbound.reshape(expert_count, capacity, model_width)
    arrived = lax.all_to_all(outbound, "sp", split_axis=0, concat_axis=0, tiled=True)
    partial_out = expert_part(
        lax.all_gather(arrived, "tp", axis=0, tiled=True), gate_proj, up_proj, down_proj
    )
    partial_out = partial_out.reshape(tp_count, expert_count * capacity, model_width)
    width_parts = lax.all_to_all(partial_out, "tp", split_axis=0, concat_axis=0, tiled=True)
    summed = jnp.sum(width_parts.astype(jnp.float32), 0).reshape(
        expert_count, capacity, model_width
    )
    returned = (
        lax.all_to_all(summed.astype(jnp.bfloat16), "sp", split_axis=0, concat_axis=0, tiled=True)
        .astype(summed.dtype)
        .reshape(expert_count * capacity, model_width)
    )
    picked = jnp.dot(
        select.astype(jnp.float32).T,
        returned,
        precision=lax.Precision.HIGHEST,
        preferred_element_type=jnp.float32,
    )
    routed = jnp.sum(picked.reshape(tok_rows, 2, model_width) * own_weights[..., None], 1)
    return (middle_f + routed).astype(jnp.bfloat16)


def solution(mesh):
    return jax.shard_map(
        per_device,
        mesh=mesh,
        in_specs=(
            P("sp", "tp"),
            P("sp", "tp"),
            P("sp", "tp"),
            P("tp"),
            P(("sp", "tp"), None),
            P("tp", None),
            P(),
            P("sp", None),
            P("sp", None),
            P("sp", None, "tp"),
            P("sp", None, "tp"),
            P("sp", "tp", None),
        ),
        out_specs=P(("sp", "tp"), None),
        check_vma=False,
    )
```
